32 devices in a mesh: sp: 8 (over z, x), dp: 4 (over y, core).
Axes of the slice: x: 2, y: 2, z: 4, core: 2. Of those that a mesh axis runs over, the one named last changes fastest.
Arguments:
- residual: bfloat16 [4, 1024, 2048], P('dp', 'sp'), may hold values from -6 to 6
- query_projected: bfloat16 [4, 1024, 1024], P('dp', 'sp'), may hold values from -6 to 6
- key_projected: bfloat16 [4, 1024, 1024], P('dp', 'sp'), may hold values from -6 to 6
- value_projected: bfloat16 [4, 1024, 1024], P('dp', 'sp'), may hold values from -6 to 6
- output_gate_proj: bfloat16 [4, 1024, 1024], P('dp', 'sp'), may hold values from -6 to 6
- write_strength_logits: float32 [4, 1024, 16], P('dp', 'sp'), may hold values from -6 to 6
- decay_logits: float32 [4, 1024, 16], P('dp', 'sp'), may hold values from -5 to 5
- extra_log_decay: float32 [4, 1024, 16], P('dp', 'sp'), may hold values from -0.7 to 0
- head_decay_rate: float32 [16], P('sp'), may hold values from 0 to 0.06
- head_norm_gain: float32 [64], replicated, may hold values from 0.1 to 1.9
- output_matrix: bfloat16 [1024, 2048], replicated, may hold values from -0.1875 to 0.1875
- expert_norm_gain: float32 [2048], replicated, may hold values from 0.1 to 1.9
- group_router_scores: float32 [4, 1024, 4], P('dp', 'sp'), may hold values from -6 to 6
- chosen_expert_scores: float32 [4, 1024, 2], P('dp', 'sp'), may hold values from -6 to 6
- routes: int32 [4, 1024, 2], P('dp', 'sp'), may hold values from 0 to 31, as said below
- gate_weight: bfloat16 [32, 2048, 1024], P(('sp', 'dp')), may hold values from -0.125 to 0.125
- up_weight: bfloat16 [32, 2048, 1024], P(('sp', 'dp')), may hold values from -0.125 to 0.125
- down_weight: bfloat16 [32, 1024, 2048], P(('sp', 'dp')), may hold values from -0.75 to 0.75
Outputs:
- layer_out: bfloat16 [4, 1024, 2048], P('dp', 'sp')
The draws below stay inside these ranges and needn't reach their ends.
Inputs may be any that keep to these rules, and one draw needn't show every extreme that they name: `routes`: the 2 numbers of a row differ and lie in one group of 8 consecutive experts. Among the rows of one device no expert is named more than 16 times, some expert exactly 16 times, and each group is named by exactly 32 rows.
All inputs are finite; a program needn't handle non-finite values.
Results may differ from the reference program's by a relative error of at most 0.0059.
Values may be sent and summed in bfloat16 or wider, within the bound.
A program may use at most 128 MiB of HBM per device.

```python
import math
import jax
import jax.numpy as jnp
from jax import lax

D = 2048
HEADS = 16
HD = 64
FF_E = 1024
GROUPS = 4
TOPK = 2
BLK = 64
TOK_DEV = 128
SEQS = 4
LEN = 1024
EXPERTS = 32


def route_block(key):
    half = 2 * TOK_DEV // EXPERTS
    per_group = EXPERTS // GROUPS
    first, second, third, fourth = jax.random.split(key, 4)
    perms = jax.vmap(lambda sub: jax.random.permutation(sub, per_group))(jax.random.split(first, GROUPS))
    expert_ids = (perms + jnp.arange(GROUPS, dtype=jnp.int32)[:, None] * per_group).astype(jnp.int32)
    deltas = jax.random.randint(second, (GROUPS, per_group // 2), 0, half + 1)
    deltas = deltas.at[0, 0].set(half)
    counts = jnp.zeros((EXPERTS,), jnp.int32)
    counts = counts.at[expert_ids[:, 0::2]].add(half + deltas)
    counts = counts.at[expert_ids[:, 1::2]].add(half - deltas)
    listed = jnp.repeat(jnp.arange(EXPERTS, dtype=jnp.int32), counts, total_repeat_length=2 * TOK_DEV)
    group_len = per_group * half
    pairs = listed.reshape(GROUPS, 2, group_len // 2).transpose(0, 2, 1).reshape(TOK_DEV, 2)
    flip = jax.random.randint(third, (TOK_DEV,), 0, 2)
    pairs = jnp.where(flip[:, None] == 1, pairs[:, ::-1], pairs)
    order = jax.random.permutation(fourth, TOK_DEV)
    return pairs[order]


def draw_routes(key, part):
    nblocks = SEQS * (LEN // TOK_DEV)
    blocks = jax.vmap(route_block)(jax.random.split(jax.random.fold_in(key, 11), nblocks))
    return blocks.reshape(SEQS, LEN, 2).astype(jnp.int32)


def draw_head_decay_rate(key, part):
    first, second = jax.random.split(jax.random.fold_in(key, 23))
    index = jax.random.permutation(first, HEADS)
    spread = jax.random.uniform(second, (HEADS,), jnp.float32)
    fast = jnp.exp(math.log(0.02) + spread * (math.log(0.06) - math.log(0.02)))
    slow = (0.1 + 0.3 * spread) / LEN
    nfast = HEADS // 2
    return jnp.where(index < nfast, fast, slow).astype(jnp.float32)


def draw_decay_logits(key, part):
    first, second = jax.random.split(jax.random.fold_in(key, 37))
    nblocks = LEN // TOK_DEV
    offset = jax.random.uniform(first, (SEQS, nblocks, 1, 1), jnp.float32, -1.0, 1.0)
    noise = jnp.clip(jax.random.normal(second, (SEQS, nblocks, TOK_DEV, HEADS), jnp.float32), -4.0, 4.0)
    return (noise + offset).reshape(SEQS, LEN, HEADS)


def draw_extra_log_decay(key, part):
    first, second = jax.random.split(jax.random.fold_in(key, 41))
    places = jax.random.randint(first, (SEQS, 2), 0, LEN)
    hit = jnp.any(jnp.arange(LEN, dtype=jnp.int32)[None, :, None] == places[:, None, :], axis=-1)
    strength = jax.random.uniform(second, (SEQS, LEN, HEADS), jnp.float32, math.log(0.5), math.log(0.8))
    return jnp.where(hit[..., None], strength, 0.0).astype(jnp.float32)


def shard_levels(own_key, extent, shards, low, largest):
    factor_of, own = 1.0, jax.random.fold_in(own_key, 6)
    for axis_at, blocks in shards:
        draws = jnp.exp(jax.random.uniform(jax.random.fold_in(own, axis_at), (blocks,), jnp.float32, low / len(shards), largest / len(shards)))
        factor_of = factor_of * jnp.repeat(draws, extent[axis_at] // blocks).reshape([-1 if axis == axis_at else 1 for axis in range(len(extent))])
    return factor_of


def normal_values(rng, extent, scale, limit, cuts=(), kind=jnp.bfloat16):
    values = scale * jax.random.normal(rng, extent, jnp.float32)
    if cuts:
        values = values * shard_levels(rng, extent, cuts, -0.22, 0.18)
    return jnp.clip(values, -limit, limit).astype(kind)


def setup_inputs(seed: int = 0) -> dict:
    streams_of = jax.random.split(jax.random.key(seed), 19)
    return {
        "residual": normal_values(streams_of[0], (SEQS, LEN, D), 1.0, 6.0, ((0, 4), (1, 8))),
        "query_projected": normal_values(streams_of[1], (SEQS, LEN, HEADS * HD), 1.0, 6.0, ((0, 4), (1, 8))),
        "key_projected": normal_values(streams_of[2], (SEQS, LEN, HEADS * HD), 1.0, 6.0, ((0, 4), (1, 8))),
        "value_projected": normal_values(streams_of[3], (SEQS, LEN, HEADS * HD), 1.0, 6.0, ((0, 4), (1, 8))),
        "output_gate_proj": normal_values(streams_of[4], (SEQS, LEN, HEADS * HD), 1.0, 6.0, ((0, 4), (1, 8))),
        "write_strength_logits": normal_values(streams_of[5], (SEQS, LEN, HEADS), 1.0, 6.0, ((0, 4), (1, 8)), jnp.float32),
        "decay_logits": draw_decay_logits(jax.random.fold_in(streams_of[18], 71), 0),
        "extra_log_decay": draw_extra_log_decay(jax.random.fold_in(streams_of[18], 71), 0),
        "head_decay_rate": draw_head_decay_rate(jax.random.fold_in(streams_of[18], 71), 0),
        "head_norm_gain": jnp.clip(1.0 + 0.18 * jax.random.normal(streams_of[9], (HD,), jnp.float32), 0.1, 1.9),
        "output_matrix": normal_values(streams_of[10], (HEADS * HD, D), (HEADS * HD) ** -0.5, 0.1875),
        "expert_norm_gain": jnp.clip(1.0 + 0.18 * jax.random.normal(streams_of[11], (D,), jnp.float32), 0.1, 1.9),
        "group_router_scores": normal_values(streams_of[12], (SEQS, LEN, GROUPS), 1.5, 6.0, ((0, 4), (1, 8)), jnp.float32),
        "chosen_expert_scores": normal_values(streams_of[13], (SEQS, LEN, TOPK), 1.0, 6.0, ((0, 4), (1, 8)), jnp.float32),
        "routes": draw_routes(jax.random.fold_in(streams_of[18], 71), 0),
        "gate_weight": normal_values(streams_of[15], (EXPERTS, D, FF_E), D ** -0.5, 0.125, ((0, 32),)),
        "up_weight": normal_values(streams_of[16], (EXPERTS, D, FF_E), D ** -0.5, 0.125, ((0, 32),)),
        "down_weight": normal_values(streams_of[17], (EXPERTS, FF_E, D), (FF_E // 16) ** -0.5, 0.75, ((0, 32),)),
    }


eps = 1e-06
block_rows = 256

def unit_rows(array):
    return array * lax.rsqrt(lax.optimization_barrier(jnp.sum(array * array, axis=-1, keepdims=True)) + eps)

def block_terms(query, keyed, valued, beta, log_decay_total, span):
    length, width = query.shape
    count = length // span
    highest_precision = lax.Precision.HIGHEST
    qb = query.reshape(count, span, width)
    kb = keyed.reshape(count, span, width)
    vb = valued.reshape(count, span, width)
    bb = beta.reshape(count, span)
    cumul = jnp.cumsum(log_decay_total.reshape(count, span), axis=1)
    rows = jnp.arange(span, dtype=jnp.int32)
    causal = rows[:, None] >= rows[None, :]
    strict = rows[:, None] > rows[None, :]
    diff = cumul[:, :, None] - cumul[:, None, :]
    decay = jnp.where(causal, jnp.exp(jnp.where(causal, diff, 0.0)), 0.0)
    kbeta = kb * bb[..., None]
    lower = jnp.where(strict, jnp.einsum('nid,njd->nij', kbeta, kb, precision=highest_precision) * decay, 0.0)
    rhs = jnp.concatenate([vb * bb[..., None], kbeta * jnp.exp(cumul)[..., None]], axis=-1)
    solved = jax.scipy.linalg.solve_triangular(lower, rhs, lower=True, unit_diagonal=True)
    state_update = solved[..., :width]
    write_decayed = solved[..., width:]
    attention_out = jnp.einsum('nid,njd->nij', qb, kb, precision=highest_precision) * decay
    query_decayed = qb * jnp.exp(cumul)[..., None]
    key_decayed = kb * jnp.exp(cumul[:, -1:] - cumul)[..., None]
    total = jnp.exp(cumul[:, -1])
    return (attention_out, query_decayed, write_decayed, state_update, key_decayed, total)

def run_head(args):
    query, keyed, valued, beta, log_decay_total = args
    length, width = query.shape
    highest_precision = lax.Precision.HIGHEST
    terms = block_terms(query, keyed, valued, beta, log_decay_total, BLK)

    def advance(state, inputs):
        attention_out, query_decayed, write_decayed, state_update, key_decayed, total = inputs
        value_corrected = state_update - jnp.dot(write_decayed, state, precision=highest_precision)
        final_output = jnp.dot(query_decayed, state, precision=highest_precision) + jnp.dot(attention_out, value_corrected, precision=highest_precision)
        state = state * total + jnp.dot(key_decayed.T, value_corrected, precision=highest_precision)
        return (state, final_output)
    _, outputs = lax.scan(advance, jnp.zeros((width, width), jnp.float32), terms)
    return outputs.reshape(length, width)

def routed(ffn_in, chosen, gate_weight, up_weight, down_weight):
    ntok, width = ffn_in.shape
    experts = gate_weight.shape[0]
    nassign = ntok * 2
    eid = chosen.reshape(nassign).astype(jnp.int32)
    order = jnp.argsort(eid, stable=True).astype(jnp.int32)
    eid_sorted = eid[order]
    counts = jnp.zeros((experts,), jnp.int32).at[eid].add(1)
    padded = (counts + block_rows - 1) // block_rows * block_rows
    start = (jnp.cumsum(counts) - counts).astype(jnp.int32)
    pend = jnp.cumsum(padded).astype(jnp.int32)
    pstart = pend - padded
    dest = pstart[eid_sorted] + jnp.arange(nassign, dtype=jnp.int32) - start[eid_sorted]
    total = nassign + experts * block_rows
    nblocks = total // block_rows
    slot_assign = jnp.full((total,), nassign, jnp.int32).at[dest].set(order)
    slot_tok = jnp.where(slot_assign < nassign, slot_assign // 2, ntok).astype(jnp.int32)
    rows = jnp.take(ffn_in, slot_tok, axis=0, mode='fill', fill_value=0).reshape(nblocks, block_rows, width)
    block_expert = jnp.minimum(jnp.searchsorted(pend, jnp.arange(nblocks, dtype=jnp.int32) * block_rows, side='right'), experts - 1).astype(jnp.int32)

    def one_block(args):
        xblock, expert = args
        gate = jnp.dot(xblock.astype(jnp.float32), gate_weight[expert].astype(jnp.float32), preferred_element_type=jnp.float32)
        upper = jnp.dot(xblock.astype(jnp.float32), up_weight[expert].astype(jnp.float32), preferred_element_type=jnp.float32)
        hidden = (jax.nn.silu(gate) * upper).astype(jnp.bfloat16)
        return jnp.dot(hidden.astype(jnp.float32), down_weight[expert].astype(jnp.float32), preferred_element_type=jnp.float32).astype(jnp.bfloat16)
    outputs = lax.map(one_block, (rows, block_expert)).reshape(total, width)
    per_assign = jnp.zeros((nassign + 1, width), jnp.bfloat16).at[slot_assign].set(outputs)[:nassign]
    return per_assign.reshape(ntok, 2, width)

def reference(residual, query_projected, key_projected, value_projected, output_gate_proj, write_strength_logits, decay_logits, extra_log_decay, head_decay_rate, head_norm_gain, output_matrix, expert_norm_gain, group_router_scores, chosen_expert_scores, routes, gate_weight, up_weight, down_weight):
    seqs, length, joined = query_projected.shape
    heads = head_decay_rate.shape[0]
    width = joined // heads
    model = residual.shape[-1]

    def heads_of(array):
        return array.astype(jnp.float32).reshape(seqs, length, heads, width).transpose(0, 2, 1, 3).reshape(seqs * heads, length, width)
    query = unit_rows(heads_of(query_projected)) * width ** (-0.5)
    keyed = unit_rows(heads_of(key_projected))
    valued = heads_of(value_projected)
    beta = jax.nn.sigmoid(write_strength_logits).transpose(0, 2, 1).reshape(seqs * heads, length)
    log_decay_total = -head_decay_rate[None, :, None] * jax.nn.softplus(decay_logits.transpose(0, 2, 1)) + extra_log_decay.transpose(0, 2, 1)
    log_decay_total = log_decay_total.reshape(seqs * heads, length)
    attended = lax.map(run_head, (query, keyed, valued, beta, log_decay_total))
    normed = attended * lax.rsqrt(lax.optimization_barrier(jnp.mean(attended * attended, axis=-1, keepdims=True)) + eps) * head_norm_gain
    normed = normed.astype(jnp.bfloat16).reshape(seqs, heads, length, width).transpose(0, 2, 1, 3).reshape(seqs * length, joined)
    gated = (normed.astype(jnp.float32) * jax.nn.silu(output_gate_proj.reshape(seqs * length, joined).astype(jnp.float32))).astype(jnp.bfloat16)
    mixed = residual.reshape(seqs * length, model).astype(jnp.float32) + jnp.dot(gated.astype(jnp.float32), output_matrix.astype(jnp.float32), preferred_element_type=jnp.float32)
    ffn_in = (mixed * lax.rsqrt(lax.optimization_barrier(jnp.mean(mixed * mixed, axis=-1, keepdims=True)) + eps) * expert_norm_gain).astype(jnp.bfloat16)
    experts = gate_weight.shape[0]
    groups = group_router_scores.shape[-1]
    per_group = experts // groups
    chosen = routes.reshape(seqs * length, 2)
    group_exp = jnp.exp(group_router_scores.reshape(seqs * length, groups))
    group_id = chosen[:, 0] // per_group
    match = jnp.arange(groups, dtype=jnp.int32)[None, :] == group_id[:, None]
    group_prob = lax.optimization_barrier(jnp.sum(jnp.where(match, group_exp, 0.0), axis=-1)) / lax.optimization_barrier(jnp.sum(group_exp, axis=-1))
    pick_exp = jnp.exp(chosen_expert_scores.reshape(seqs * length, 2))
    weight = group_prob[:, None] * pick_exp / lax.optimization_barrier(jnp.sum(pick_exp, axis=-1, keepdims=True))
    expert_out = routed(ffn_in, chosen, gate_weight, up_weight, down_weight)
    moe = lax.optimization_barrier(jnp.sum(weight[..., None] * expert_out.astype(jnp.float32), axis=1))
    return (mixed + moe).astype(jnp.bfloat16).reshape(seqs, length, model)
```

```python
import functools

import jax
import jax.numpy as jnp
from jax import lax
from jax.experimental import pallas as pl
from jax.experimental.pallas import tpu as pltpu
from jax.sharding import PartitionSpec as P

BLK = 64


eps = 1e-06


def split_two(array):
    high = array.astype(jnp.bfloat16)
    low = (array - high.astype(jnp.float32)).astype(jnp.bfloat16)
    return high, low


def contract(left, right, dims):
    return lax.dot_general(left, right, (dims, ((), ())), preferred_element_type=jnp.float32)


NN = ((1,), (0,))
NT = ((1,), (1,))
TN = ((0,), (0,))


def dot_fine(left, right, dims=NN):
    left_high, left_low = split_two(left)
    right_high, right_low = split_two(right)
    return contract(left_high, right_high, dims) + (
        contract(left_high, right_low, dims) + contract(left_low, right_high, dims)
    )


def mixer_kernel(
    tok, width, heads_here, per_step,
    x_ref, row_ref, col_ref, gain_ref, out_ref, map_ref, add_ref, qe_ref, base_ref,
):
    count = row_ref.shape[0]
    span = BLK
    size = heads_here * span
    lanes = heads_here * width
    per_tok = tok // span
    rows = lax.broadcasted_iota(jnp.int32, (size, size), 0)
    cols = lax.broadcasted_iota(jnp.int32, (size, size), 1)
    same = (rows // span) == (cols // span)
    causal = same & (rows >= cols)
    strict = same & (rows > cols)
    own = (lax.broadcasted_iota(jnp.int32, (size, lanes), 0) // span) == (
        lax.broadcasted_iota(jnp.int32, (size, lanes), 1) // width
    )
    diag_rows = lax.broadcasted_iota(jnp.int32, (lanes, lanes), 0)
    diag_cols = lax.broadcasted_iota(jnp.int32, (lanes, lanes), 1)
    unit = (diag_rows == diag_cols).astype(jnp.float32)
    eye = (rows == cols).astype(jnp.float32)

    def stacked(block):
        block = block.astype(jnp.float32)
        return jnp.where(own, jnp.concatenate([block] * heads_here, axis=0), 0.0)

    def unit_rows(array):
        return array * lax.rsqrt(jnp.sum(array * array, axis=-1, keepdims=True) + eps)

    def terms(step, carry):
        held = []
        for inner in range(per_step):
            chunk = step * per_step + inner
            source = chunk // per_tok
            offset = (chunk % per_tok) * span
            query = unit_rows(stacked(x_ref[source, pl.ds(offset, span), :])) * width ** (-0.5)
            keyed = unit_rows(stacked(x_ref[source, pl.ds(tok + offset, span), :]))
            valued = stacked(x_ref[source, pl.ds(2 * tok + offset, span), :])
            column = col_ref[chunk]
            beta, cumul = column[:, 0:1], column[:, 1:2]
            grown, remaining, total = column[:, 2:3], column[:, 3:4], column[:, 4:5]
            diff = cumul - row_ref[chunk][1:2, :]
            decay = jnp.where(causal, jnp.exp(jnp.where(causal, diff, 0.0)), 0.0)
            kbeta = keyed * beta
            lower = jnp.where(strict, dot_fine(kbeta, keyed, NT) * decay, 0.0)
            attention = dot_fine(query, keyed, NT) * decay
            held.append((chunk, query, keyed, valued, beta, grown, remaining, total, kbeta, lower, attention))
        inverses = [
            eye - jnp.where((rows // 2) == (cols // 2), each[9], 0.0) for each in held
        ]
        level = 2
        while level < span:
            mask = ((rows // (2 * level)) == (cols // (2 * level))) & ((rows // level) != (cols // level))
            first = [
                dot_fine(jnp.where(mask, each[9], 0.0), inverse)
                for each, inverse in zip(held, inverses)
            ]
            inverses = [
                inverse - dot_fine(inverse, part) for inverse, part in zip(inverses, first)
            ]
            level *= 2
        for each, inverse in zip(held, inverses):
            chunk, query, keyed, valued, beta, grown, remaining, total, kbeta, lower, attention = each
            update = dot_fine(inverse, valued * beta)
            written = dot_fine(inverse, kbeta * grown)
            faded = keyed * remaining
            map_ref[chunk] = unit * total - dot_fine(faded, written, TN)
            add_ref[chunk] = dot_fine(faded, update, TN)
            qe_ref[chunk] = query * grown - dot_fine(attention, written)
            base_ref[chunk] = dot_fine(attention, update)
        return carry

    lax.fori_loop(0, count // per_step, terms, 0)
    gain = gain_ref[...]

    def advance(source, state):
        for inner in range(per_tok):
            chunk = source * per_tok + inner
            attended = dot_fine(qe_ref[chunk], state) + base_ref[chunk]
            state = dot_fine(map_ref[chunk], state) + add_ref[chunk]
            mean = jnp.sum(attended * attended, axis=-1, keepdims=True) / width
            normed = attended * lax.rsqrt(mean + eps) * gain
            joined = normed[:span]
            for head in range(1, heads_here):
                joined = joined + normed[head * span : (head + 1) * span]
            out_ref[source, inner * span : (inner + 1) * span, :] = joined.astype(out_ref.dtype)
        return state

    lax.fori_loop(0, count // per_tok, advance, jnp.zeros((lanes, lanes), jnp.float32))


def mixer(arrived, rows, cols, gain, tok, width, heads_here):
    sources = arrived.shape[0]
    count, _, size = rows.shape
    lanes = heads_here * width
    return pl.pallas_call(
        functools.partial(mixer_kernel, tok, width, heads_here, 4),
        out_shape=jax.ShapeDtypeStruct((sources, tok, lanes), jnp.bfloat16),
        in_specs=[pl.BlockSpec(memory_space=pltpu.VMEM)] * 4,
        out_specs=pl.BlockSpec(memory_space=pltpu.VMEM),
        scratch_shapes=[
            pltpu.VMEM((count, lanes, lanes), jnp.float32),
            pltpu.VMEM((count, lanes, lanes), jnp.float32),
            pltpu.VMEM((count, size, lanes), jnp.float32),
            pltpu.VMEM((count, size, lanes), jnp.float32),
        ],
    )(arrived, rows, cols, gain)


def expert_apply(rows, gate_weight, up_weight, down_weight):
    gate = jnp.dot(rows, gate_weight[0], preferred_element_type=jnp.float32)
    upper = jnp.dot(rows, up_weight[0], preferred_element_type=jnp.float32)
    hidden = (jax.nn.silu(gate) * upper).astype(jnp.bfloat16)
    return jnp.dot(hidden, down_weight[0], preferred_element_type=jnp.float32).astype(jnp.bfloat16)


def three_pieces(array):
    first = lax.reduce_precision(array, 8, 7)
    second = lax.reduce_precision(array - first, 8, 7)
    third = lax.reduce_precision(array - first - second, 8, 7)
    return first.astype(jnp.bfloat16), second.astype(jnp.bfloat16), third.astype(jnp.bfloat16)


def rank_of(named):
    length = named.shape[0]
    index = jnp.arange(length, dtype=jnp.int32)
    before = (index[:, None] > index[None, :]).astype(jnp.bfloat16)
    return jnp.dot(before, named.astype(jnp.bfloat16), preferred_element_type=jnp.float32).astype(
        jnp.int32
    )


def shards(
    residual,
    query_projected,
    key_projected,
    value_projected,
    output_gate_proj,
    write_strength_logits,
    decay_logits,
    extra_log_decay,
    head_decay_rate,
    head_norm_gain,
    output_matrix,
    expert_norm_gain,
    group_router_scores,
    chosen_expert_scores,
    routes,
    gate_weight,
    up_weight,
    down_weight,
):
    sp_count = lax.axis_size("sp")
    dp_count = lax.axis_size("dp")
    heads_here = head_decay_rate.shape[0]
    width = head_norm_gain.shape[0]
    tok = residual.shape[1]
    model = residual.shape[2]
    lanes = heads_here * width
    length = sp_count * tok
    count = length // BLK

    def by_owner(array):
        return array[0].reshape(tok, sp_count, lanes).transpose(1, 0, 2)

    scalars = jnp.stack([write_strength_logits[0], decay_logits[0], extra_log_decay[0]])
    pieces = jnp.stack(three_pieces(scalars))
    pieces = pieces.reshape(3, 3, tok, sp_count, heads_here).transpose(3, 0, 1, 4, 2)
    pieces = pieces.reshape(sp_count, -1, lanes)
    used = pieces.shape[1]
    pieces = jnp.pad(pieces, ((0, 0), (0, -used % 16), (0, 0)))
    packed = jnp.concatenate(
        [by_owner(query_projected), by_owner(key_projected), by_owner(value_projected), pieces],
        axis=1,
    )
    arrived = lax.all_to_all(packed, "sp", split_axis=0, concat_axis=0, tiled=True)
    scalars = arrived[:, 3 * tok : 3 * tok + used].astype(jnp.float32)
    scalars = scalars.reshape(sp_count, 3, 3, heads_here, tok)
    scalars = (scalars[:, 0] + scalars[:, 1]) + scalars[:, 2]
    scalars = scalars.transpose(1, 2, 0, 3).reshape(3, heads_here, count, BLK).transpose(0, 2, 1, 3)
    beta = jax.nn.sigmoid(scalars[0])
    log_decay = -head_decay_rate[None, :, None] * jax.nn.softplus(scalars[1]) + scalars[2]
    index = jnp.arange(BLK, dtype=jnp.int32)
    upto = (index[:, None] <= index[None, :]).astype(jnp.float32)
    cumul = jnp.dot(log_decay, upto, precision=lax.Precision.HIGHEST)
    last = cumul[..., -1:]
    total = jnp.broadcast_to(jnp.exp(last), cumul.shape)
    spare = jnp.zeros_like(cumul)
    rows = jnp.stack(
        [beta, cumul, jnp.exp(cumul), jnp.exp(last - cumul), total, spare, spare, spare], axis=1
    ).reshape(count, 8, heads_here * BLK)
    cols = rows.transpose(0, 2, 1)
    gain = jnp.tile(head_norm_gain, heads_here)[None, :]
    normed = mixer(arrived, rows, cols, gain, tok, width, heads_here)
    returned = lax.all_to_all(normed, "sp", split_axis=0, concat_axis=0, tiled=True)
    returned = returned.transpose(1, 0, 2).reshape(tok, sp_count * lanes)
    gated = (
        returned.astype(jnp.float32) * jax.nn.silu(output_gate_proj[0].astype(jnp.float32))
    ).astype(jnp.bfloat16)
    mixed = residual[0].astype(jnp.float32) + jnp.dot(
        gated, output_matrix, preferred_element_type=jnp.float32
    )
    ffn_in = (
        mixed * lax.rsqrt(jnp.mean(mixed * mixed, axis=-1, keepdims=True) + eps) * expert_norm_gain
    ).astype(jnp.bfloat16)

    experts = sp_count * dp_count
    groups = group_router_scores.shape[-1]
    per_group = experts // groups
    share = tok // groups
    capacity = groups * (4 * tok // experts)
    chosen = routes[0]
    group_exp = jnp.exp(group_router_scores[0])
    group_id = chosen[:, 0] // per_group
    group_range = jnp.arange(groups, dtype=jnp.int32)
    match = group_range[None, :] == group_id[:, None]
    group_prob = jnp.sum(jnp.where(match, group_exp, 0.0), axis=-1) / jnp.sum(group_exp, axis=-1)
    pick_exp = jnp.exp(chosen_expert_scores[0])
    weight = group_prob[:, None] * pick_exp / jnp.sum(pick_exp, axis=-1, keepdims=True)
    local_id = (chosen - group_id[:, None] * per_group).astype(jnp.bfloat16)
    notes = jnp.concatenate((local_id,) + three_pieces(weight), axis=1)
    notes = jnp.pad(notes, ((0, 0), (0, 128 - notes.shape[1])))

    group_rank = rank_of(match)
    place = (
        match[:, :, None]
        & (group_rank[:, :, None] == jnp.arange(share, dtype=jnp.int32)[None, None, :])
    ).reshape(tok, tok).astype(jnp.bfloat16)
    outgoing = contract(place, jnp.concatenate([ffn_in, notes], axis=1), TN).astype(jnp.bfloat16)
    across = [[member + group * per_group for group in range(groups)] for member in range(per_group)]
    within = [[group * per_group + member for member in range(per_group)] for group in range(groups)]
    axes = ("sp", "dp")
    held = lax.all_to_all(
        outgoing, axes, split_axis=0, concat_axis=0, tiled=True, axis_index_groups=across
    )
    held_rows, held_notes = held[:, :model], held[:, model:].astype(jnp.float32)
    ids = held_notes[:, 0:2].astype(jnp.int32)
    weights = (held_notes[:, 2:4] + held_notes[:, 4:6]) + held_notes[:, 6:8]
    hits = ids[:, :, None] == jnp.arange(per_group, dtype=jnp.int32)[None, None, :]
    named = hits[:, 0] | hits[:, 1]
    expert_weight = jnp.sum(jnp.where(hits, weights[:, :, None], 0.0), axis=1)
    expert_rank = rank_of(named)
    seat = named[:, :, None] & (
        expert_rank[:, :, None] == jnp.arange(capacity, dtype=jnp.int32)[None, None, :]
    )
    seat_weight = jnp.where(seat, expert_weight[:, :, None], 0.0).reshape(tok, -1)
    seated = contract(
        seat.reshape(tok, -1).astype(jnp.bfloat16), held_rows, TN
    ).astype(jnp.bfloat16)
    produced = expert_apply(
        lax.all_to_all(
            seated, axes, split_axis=0, concat_axis=0, tiled=True, axis_index_groups=within
        ),
        gate_weight,
        up_weight,
        down_weight,
    )
    came_back = lax.all_to_all(
        produced, axes, split_axis=0, concat_axis=0, tiled=True, axis_index_groups=within
    )
    weight_high = lax.reduce_precision(seat_weight, 8, 7)
    weight_low = (seat_weight - weight_high).astype(jnp.bfloat16)
    summed = contract(weight_high.astype(jnp.bfloat16), came_back, NN) + contract(
        weight_low, came_back, NN
    )
    home = lax.all_to_all(
        summed.astype(jnp.bfloat16),
        axes,
        split_axis=0,
        concat_axis=0,
        tiled=True,
        axis_index_groups=across,
    )
    moe = contract(place, home, NN)
    return (mixed + moe).astype(jnp.bfloat16)[None]


def solution(mesh):
    in_specs = (
        P("dp", "sp", None),
        P("dp", "sp", None),
        P("dp", "sp", None),
        P("dp", "sp", None),
        P("dp", "sp", None),
        P("dp", "sp", None),
        P("dp", "sp", None),
        P("dp", "sp", None),
        P("sp"),
        P(),
        P(),
        P(),
        P("dp", "sp", None),
        P("dp", "sp", None),
        P("dp", "sp", None),
        P(("sp", "dp"), None, None),
        P(("sp", "dp"), None, None),
        P(("sp", "dp"), None, None),
    )
    out_specs = P("dp", "sp", None)
    return jax.shard_map(shards, mesh=mesh, in_specs=in_specs, out_specs=out_specs, check_vma=False)
```
